32 devices in a mesh: fs: 8 (over z, y), tp: 4 (over x, core).
Axes of the slice: x: 2, y: 2, z: 4, core: 2. Of those that a mesh axis runs over, the one named last changes fastest.
Arguments:
- normed_input: bfloat16 [6144, 2048], P(('fs', 'tp')), may hold values from -6 to 6
- pre_act: bfloat16 [6144, 8192], P('fs', 'tp'), may hold values from -6 to 6
- out_grad: bfloat16 [6144, 2048], P(('fs', 'tp')), may hold values from -6 to 6
- up_weight: bfloat16 [2048, 8192], P('fs', 'tp'), may hold values from -0.125 to 0.125
- down_weight: bfloat16 [8192, 2048], P('tp', 'fs'), may hold values from -0.0625 to 0.0625
Outputs:
- input_grad: bfloat16 [6144, 2048], P(('fs', 'tp'))
- up_grad: float32 [2048, 8192], P('fs', 'tp')
- down_grad: float32 [8192, 2048], P('tp', 'fs')
The draws below stay inside these ranges and needn't reach their ends.
All inputs are finite; a program needn't handle non-finite values.
Results may differ from the reference program's by a relative error of at most 0.014.
Values may be sent and summed in bfloat16 or wider, within the bound.
No kernel may reach another device: no remote copies, remote signals or barrier semaphores. Data moves between devices by JAX's collectives and lax.ppermute only.
A program may use at most 128 MiB of HBM per device.

```python
import jax
import jax.numpy as jnp
from jax import lax

D = 2048
FF = 8192
TOKENS = 6144
N_TP = 4


def raised(values, stream_key, source, target, blocks, factor):
    owner, partner = [(jnp.arange(values.shape[dim]) // (values.shape[dim] // blocks)).reshape([-1 if axis == dim else 1 for axis in range(values.ndim)]) for dim in (source, target)]
    chosen = jax.random.permutation(stream_key, blocks)[partner]
    strong = (owner == chosen) | (owner == (partner + blocks // 2) % blocks)
    return jnp.where(strong, factor * values, values)


def shard_levels(stream_key, extent, split, smallest, high):
    gain, own = 1.0, jax.random.fold_in(stream_key, 6)
    for position, shards_of in split:
        steps = jnp.exp(jax.random.uniform(jax.random.fold_in(own, position), (shards_of,), jnp.float32, smallest / len(split), high / len(split)))
        gain = gain * jnp.repeat(steps, extent[position] // shards_of).reshape([-1 if axis == position else 1 for axis in range(len(extent))])
    return gain


def centred(key, shape, scale, limit, cuts=(), dtype=jnp.bfloat16):
    drawn = jax.random.normal(key, shape, jnp.float32) * scale
    if len(cuts) > 0:
        drawn = shard_levels(key, shape, cuts, -0.22, 0.18) * drawn
    return jnp.clip(drawn, min=-limit, max=limit).astype(dtype)


def heavy_noise(stream_key, dims, spread, most, cuts, heavy, kind=jnp.bfloat16):
    result = spread * jax.random.normal(stream_key, dims, jnp.float32)
    if cuts:
        result = result * shard_levels(stream_key, dims, cuts, -0.22, 0.18)
    return jnp.clip(raised(result, jax.random.fold_in(stream_key, 3), *heavy), -most, most).astype(kind)


def setup_inputs(seed: int = 0) -> dict:
    streams_of = jax.random.split(jax.random.key(seed), 6)
    normed_input = centred(streams_of[0], (TOKENS, D), 1.0, 6.0, ((0, 32),))
    pre_act = centred(streams_of[1], (TOKENS, FF), 1.0, 6.0, ((0, 8), (1, 4)))
    out_grad = heavy_noise(streams_of[2], (TOKENS, D), 1.0, 6.0, ((0, 32),), (0, 1, 32, 2.75))
    up_weight = centred(streams_of[3], (D, FF), D ** -0.5, 0.125, ((0, 8), (1, 4)))
    down_weight = centred(streams_of[4], (FF, D), FF ** -0.5, 0.0625, ((0, 4), (1, 8)))
    return {"normed_input": normed_input, "pre_act": pre_act, "out_grad": out_grad, "up_weight": up_weight, "down_weight": down_weight}


def reference(normed_input, pre_act, out_grad, up_weight, down_weight):
    active = jnp.maximum(pre_act.astype(jnp.float32), 0.0)
    hidden = (active * active).astype(jnp.bfloat16)
    width = FF // N_TP
    up_blocks = up_weight.reshape(D, N_TP, width).transpose(1, 0, 2)
    down_blocks = down_weight.reshape(N_TP, width, D)
    act_blocks = active.reshape(TOKENS, N_TP, width).transpose(1, 0, 2)
    hid_blocks = hidden.reshape(TOKENS, N_TP, width).transpose(1, 0, 2)

    def one_block(items):
        up_part, down_part, act_part, hid_part = items
        grad_hidden = jnp.dot(out_grad, down_part.T, preferred_element_type=jnp.float32)
        pre_grad = (2.0 * act_part * grad_hidden).astype(jnp.bfloat16)
        part = jnp.dot(pre_grad, up_part.T, preferred_element_type=jnp.float32).astype(jnp.bfloat16)
        up_part_grad = jnp.dot(normed_input.T, pre_grad, preferred_element_type=jnp.float32)
        down_part_grad = jnp.dot(hid_part.T, out_grad, preferred_element_type=jnp.float32)
        return part, up_part_grad, down_part_grad

    parts, up_grads, down_grads = lax.map(one_block, (up_blocks, down_blocks, act_blocks, hid_blocks))
    input_grad = jnp.sum(parts.astype(jnp.float32), axis=0).astype(jnp.bfloat16)
    up_grad = up_grads.transpose(1, 0, 2).reshape(D, FF)
    down_grad = down_grads.reshape(FF, D)
    return input_grad, up_grad, down_grad
```

```python
import jax
import jax.numpy as jnp
from jax import lax
from jax.sharding import PartitionSpec as P


def solution(mesh):
    n_fs = mesh.shape["fs"]
    n_tp = mesh.shape["tp"]
    lanes = [[2 * q + p for q in range(n_fs // 2)] for p in range(2)]
    pair = [(f, f ^ 1) for f in range(n_fs)]
    bits = [1 << b for b in reversed(range((n_tp - 1).bit_length()))]
    masks = [0]
    for bit in bits:
        masks = masks + [m ^ bit for m in masks]

    def swap_fs(a):
        return lax.ppermute(a, "fs", pair)

    def swap_tp(a, bit):
        return lax.ppermute(a, "tp", [(t, t ^ bit) for t in range(n_tp)])

    def local(normed_input, pre_act, out_grad, up_weight, down_weight):
        y = lax.axis_index("fs") % 2
        t = lax.axis_index("tp")
        rows, width = pre_act.shape
        half = width // 2
        block = rows // n_tp
        d_model = out_grad.shape[1]
        f32, bf16 = jnp.float32, jnp.bfloat16

        def ordered(own, other, axis):
            return jnp.where(
                y == 0,
                jnp.concatenate([own, other], axis=axis),
                jnp.concatenate([other, own], axis=axis),
            )

        def down_half(s):
            return lax.dynamic_slice_in_dim(down_weight, s * half, half, 0)

        def up_half(s):
            return lax.dynamic_slice_in_dim(up_weight, s * half, half, 1)

        down_two = ordered(down_half(y), swap_fs(down_half(1 - y)), 1)
        down_full = lax.all_gather(down_two, "fs", axis=1, tiled=True, axis_index_groups=lanes)
        up_two = ordered(up_half(y), swap_fs(up_half(1 - y)), 0)
        up_full = lax.all_gather(up_two, "fs", axis=0, tiled=True, axis_index_groups=lanes)

        def tokens(a):
            s = jnp.stack([a, swap_fs(a)])[:, None]
            for bit in bits:
                s = jnp.concatenate([s, swap_tp(s, bit)], axis=1)
            return s.reshape(2 * rows, d_model)

        grad_rows = tokens(out_grad)
        in_rows = tokens(normed_input)

        def act_half(s):
            return jnp.concatenate(
                [
                    lax.dynamic_slice(pre_act, ((t ^ m) * block, s * half), (block, half))
                    for m in masks
                ],
                axis=0,
            )

        act = jnp.concatenate([act_half(y), swap_fs(act_half(1 - y))], axis=0)
        active = jnp.maximum(act.astype(f32), 0.0)
        hidden = (active * active).astype(bf16)

        def scattered(left, right):
            part = jnp.dot(left.T, right, preferred_element_type=f32).astype(bf16)
            return lax.psum_scatter(
                part, "fs", scatter_dimension=0, tiled=True, axis_index_groups=lanes
            )

        def joined(mine):
            quarter = mine.shape[0] // 2
            keep = lax.dynamic_slice_in_dim(mine, y * quarter, quarter, 0)
            send = lax.dynamic_slice_in_dim(mine, (1 - y) * quarter, quarter, 0)
            return ordered(keep, swap_fs(send), 1).astype(f32)

        hidden_grad = jnp.dot(grad_rows, down_full.T, preferred_element_type=f32)
        pre_grad = (2.0 * active * hidden_grad).astype(bf16)
        down_mine = scattered(grad_rows, hidden)
        up_mine = scattered(in_rows, pre_grad)

        s = jnp.dot(pre_grad, up_full.T, preferred_element_type=f32).astype(bf16)
        s = s.reshape(2, n_tp, block, d_model)
        for bit in reversed(bits):
            n = s.shape[1] // 2
            s = (s[:, :n].astype(f32) + swap_tp(s[:, n:], bit).astype(f32)).astype(bf16)
        input_grad = (s[0, 0].astype(f32) + swap_fs(s[1, 0]).astype(f32)).astype(bf16)
        return input_grad, joined(up_mine), joined(down_mine).T

    placed = (
        P(("fs", "tp"), None),
        P("fs", "tp"),
        P(("fs", "tp"), None),
        P("fs", "tp"),
        P("tp", "fs"),
    )
    return jax.shard_map(
        local,
        mesh=mesh,
        in_specs=placed,
        out_specs=(P(("fs", "tp"), None), P("fs", "tp"), P("tp", "fs")),
        check_vma=False,
    )
```
